128 devices in a mesh: ep: 64 (over z, y, x), tp: 2 (over core).
Axes of the slice: x: 4, y: 4, z: 4, core: 2. Of those that a mesh axis runs over, the one named last changes fastest.
Arguments:
- hidden_in: bfloat16 [2048, 2048], P('ep'), may hold values from -6 to 6
- past_lengths: int32 [2048], P('ep'), may hold values from 1 to 1023, as said below
- key_cache: bfloat16 [2048, 1024, 256], P('ep', None, 'tp'), may hold values from -512 to 512
- value_cache: bfloat16 [2048, 1024, 256], P('ep', None, 'tp'), may hold values from -6 to 6
- attn_gain: float32 [2048], replicated, may hold values from 0.1 to 1.9
- w_query: bfloat16 [2048, 2048], P(None, 'tp'), may hold values from -0.125 to 0.125
- w_key: bfloat16 [2048, 256], P(None, 'tp'), may hold values from -0.125 to 0.125
- w_value: bfloat16 [2048, 256], P(None, 'tp'), may hold values from -0.125 to 0.125
- lambdas: float32 [16], P('tp'), may hold values from 0.3 to 0.8
- head_gain: float32 [128], replicated, may hold values from 0.1 to 1.9
- w_out: bfloat16 [2048, 2048], P('tp'), may hold values from -0.125 to 0.125
- ffn_gain: float32 [2048], replicated, may hold values from 0.1 to 1.9
- route_ids: int32 [2048, 2], P('ep'), may hold values from 0 to 31, all different within a row; in each aligned block of 32 rows (0 to 31, 32 to 63, ...) at most 4 rows name the same one
- route_weights: float32 [2048, 2], P('ep'), may hold values from 0.2 to 1
- expert_gate: bfloat16 [64, 2048, 704], P('ep', None, 'tp'), may hold values from -0.125 to 0.125
- expert_up: bfloat16 [64, 2048, 704], P('ep', None, 'tp'), may hold values from -0.125 to 0.125
- expert_down: bfloat16 [64, 704, 2048], P('ep', None, 'tp'), may hold values from -1.25 to 1.25
- gate_vector: bfloat16 [2048], replicated, may hold values from -0.125 to 0.125
- dense_gate: bfloat16 [2048, 5632], P(None, ('ep', 'tp')), may hold values from -0.125 to 0.125
- dense_up: bfloat16 [2048, 5632], P(None, ('ep', 'tp')), may hold values from -0.125 to 0.125
- dense_down: bfloat16 [5632, 2048], P('ep', 'tp'), may hold values from -0.625 to 0.625
Outputs:
- mixed_out: bfloat16 [2048, 2048], P('ep', 'tp')
- new_keys: bfloat16 [2048, 256], P('ep', 'tp')
- new_values: bfloat16 [2048, 256], P('ep', 'tp')
The draws below stay inside these ranges and needn't reach their ends.
Inputs may be any that keep to these rules, and one draw needn't show every extreme that they name: `past_lengths`: the new token of a sequence stands at this position; some sequence has 1023 cached positions in every draw. `route_ids`: each row names 2 different experts; among the rows of one index of ep no expert is named more than 4 times, a bound that some block reaches in every draw.
All inputs are finite; a program needn't handle non-finite values.
Results may differ from the reference program's by a relative error of at most 0.02.
The reference program's roundings to bfloat16 on the way count: a program that leaves them out, or rounds other values in their place, can miss the bound.
Values may be sent and summed in bfloat16 or wider, within the bound.
No kernel may reach another device: no remote copies, remote signals or barrier semaphores. Data moves between devices by JAX's collectives and lax.ppermute only.
A program may use at most 128 MiB of HBM per device.

```python
import math
import jax
import jax.numpy as jnp
import numpy as np
from jax import lax

D = 2048
HEADS = 16
KV_HEADS = 2
HEAD_DIM = 64
VALUE_DIM = 128
EXPERT_W = 1408
FF_DENSE = 5632
TOP = 2
CACHE_LEN = 1024
SEQ_GRP = 32
EXPERTS = 32
CAP = 4
SEQS = 2048
N_EP = 64
N_TP = 2


def draw_past_lengths(key, part):
    key_top, key_share, key_pick = jax.random.split(jax.random.fold_in(key, 71), 3)
    groups = SEQS // SEQ_GRP
    reach_top = jax.random.randint(key_top, (groups, 1), CACHE_LEN // 8, CACHE_LEN)
    shares = jax.random.randint(key_share, (groups, SEQ_GRP), 0, 65536)
    lengths = (1 + (reach_top - 1) * shares // 65536).reshape(-1)
    chosen = jax.random.randint(key_pick, (), 0, SEQS)
    return jnp.where(jnp.arange(SEQS) == chosen, CACHE_LEN - 1, lengths).astype(jnp.int32)


def draw_key_cache(key, part):
    key_drawn = jax.random.fold_in(jax.random.fold_in(key, 73), 0)
    extent = (SEQS, CACHE_LEN, KV_HEADS * 2 * HEAD_DIM)
    drawn_keys = jax.random.truncated_normal(key_drawn, -4.0, 4.0, extent, jnp.float32) * 1.7
    return drawn_keys.astype(jnp.bfloat16)


def shard_levels(own_key, dims, cuts, least, high):
    loudness = 1.0
    for dim, blocks in cuts:
        draws = jax.random.uniform(jax.random.fold_in(jax.random.fold_in(own_key, 6), dim), (blocks,), jnp.float32, least / len(cuts), high / len(cuts))
        loudness = loudness * jnp.repeat(jnp.exp(draws), dims[dim] // blocks).reshape((-1,) + (1,) * (len(dims) - 1 - dim))
    return loudness


def routed_block(stream_key, own, number, rows, number_of, top, limit, slope):
    sequence = jax.random.permutation(stream_key, number_of)
    crowded, usual = portions_of(number_of, rows * top, limit, slope, True), portions_of(number_of, rows * top, limit, slope, False)
    places = jnp.arange(number_of)

    def named(sizes, turn):
        used = int((sizes > 0).sum())
        fixed = max(1, used // 4)
        moved = fixed + (places - fixed + turn * (used - fixed)) % max(1, number_of - fixed)
        return jnp.zeros((number_of,), jnp.int32).at[sequence[jnp.where(places < fixed, places, moved)]].set(jnp.asarray(sizes, jnp.int32))

    sizes = jnp.where(number % 4 == 0, named(crowded, number // 4), named(usual, number - number // 4 - 1))
    mixed = jax.random.permutation(jax.random.fold_in(own, 3), number_of)
    giver, sink = mixed[0:number_of // 2 * 2:2], mixed[1:number_of // 2 * 2:2]
    room = jnp.minimum(sizes[giver] - 1, limit - sizes[sink]) // 2
    room = jnp.where((giver == sequence[0]) | (sink == sequence[0]) | (sizes[sink] == 0), 0, jnp.maximum(room, 0))
    moved = jax.random.randint(jax.random.fold_in(own, 4), (number_of // 2,), 0, 1 << 20) % (room + 1)
    sizes = sizes.at[giver].add(-moved).at[sink].add(moved)
    items = jnp.searchsorted(jnp.cumsum(sizes), jnp.arange(rows * top), side="right").astype(jnp.int32)
    grid = items.reshape(top, rows).T
    grid = grid[jax.random.permutation(jax.random.fold_in(own, 1), rows)]
    turn = jax.random.randint(jax.random.fold_in(own, 2), (rows, 1), 0, top)
    return jnp.take_along_axis(grid, (jnp.arange(top)[None, :] + turn) % top, axis=1)


def portions_of(amount, total, limit, slope, full):
    loads = [(1 << 20) // math.isqrt(rank ** slope) + 1 for rank in range(1, amount + 1)]
    largest = limit if full else min(limit, max(-(-total // amount), total * loads[0] // sum(loads)))
    least = 1 if total - largest >= amount - 1 else 0
    given, spare = [largest] + [least] * (amount - 1), total - largest - least * (amount - 1)
    while spare > 0:
        movable = [i for i in range(1, amount) if given[i] < largest] or [i for i in range(1, amount) if given[i] < limit]
        pool, left = sum([loads[i] for i in movable]), spare
        for i in movable:
            addition = min(limit - given[i], max(1, left * loads[i] // pool), spare)
            given[i] = given[i] + addition
            spare = spare - addition
    return np.array(given)


def noise(own_key, shape, spread, bound, pieces=(), held_as=jnp.bfloat16):
    gain = shard_levels(own_key, shape, pieces, -0.22, 0.18) if pieces else 1.0
    values = jax.random.normal(own_key, shape, jnp.float32) * spread * gain
    return jnp.minimum(jnp.maximum(values, -bound), bound).astype(held_as)


def setup_inputs(seed: int = 0) -> dict:
    key_of = jax.random.split(jax.random.key(seed), 22)
    hidden_in = noise(key_of[0], (SEQS, D), 1.0, 6.0, ((0, 64),))
    past_lengths = draw_past_lengths(jax.random.fold_in(key_of[21], 71), 0)
    key_cache = draw_key_cache(jax.random.fold_in(key_of[21], 71), 0)
    value_cache = noise(key_of[3], (SEQS, CACHE_LEN, KV_HEADS * VALUE_DIM), 1.0, 6.0, ((0, 64), (2, 2)))
    attn_gain = jnp.clip(1.0 + 0.18 * jax.random.normal(key_of[4], (D,), jnp.float32), 0.1, 1.9)
    w_query = noise(key_of[5], (D, HEADS * 2 * HEAD_DIM), D ** -0.5, 0.125, ((1, 2),))
    w_key = noise(key_of[6], (D, KV_HEADS * 2 * HEAD_DIM), D ** -0.5, 0.125, ((1, 2),))
    w_value = noise(key_of[7], (D, KV_HEADS * VALUE_DIM), D ** -0.5, 0.125, ((1, 2),))
    lambdas = jnp.clip(0.3 + 0.5 * jax.random.uniform(key_of[8], (HEADS,), jnp.float32) ** shard_levels(key_of[8], (HEADS,), ((0, 2),), -0.2, 0.2), 0.3, 0.8)
    head_gain = jnp.clip(1.0 + 0.18 * jax.random.normal(key_of[9], (VALUE_DIM,), jnp.float32), 0.1, 1.9)
    w_out = noise(key_of[10], (HEADS * VALUE_DIM, D), (HEADS * VALUE_DIM) ** -0.5, 0.125, ((0, 2),))
    ffn_gain = jnp.clip(1.0 + 0.18 * jax.random.normal(key_of[11], (D,), jnp.float32), 0.1, 1.9)
    route_ids_keys = jax.random.split(jax.random.fold_in(key_of[12], 1), SEQS // SEQ_GRP)
    route_ids_turns = jax.random.permutation(jax.random.fold_in(key_of[12], 3), SEQS // SEQ_GRP)
    route_ids = jax.vmap(lambda own, number: routed_block(jax.random.fold_in(key_of[12], 2), own, number, SEQ_GRP, EXPERTS, TOP, CAP, 2))(route_ids_keys, route_ids_turns).reshape((SEQS, TOP))
    route_weights = jnp.clip(0.2 + 0.8 * jax.random.uniform(key_of[13], (SEQS, TOP), jnp.float32) ** shard_levels(key_of[13], (SEQS, TOP), ((0, 64),), -0.2, 0.2), 0.2, 1.0)
    expert_gate = noise(key_of[14], (2 * EXPERTS, D, EXPERT_W // 2), D ** -0.5, 0.125, ((0, 64), (2, 2)))
    expert_up = noise(key_of[15], (2 * EXPERTS, D, EXPERT_W // 2), D ** -0.5, 0.125, ((0, 64), (2, 2)))
    expert_down = noise(key_of[16], (2 * EXPERTS, EXPERT_W // 2, D), (3.0 * EXPERT_W ** -0.5), 1.25, ((0, 64), (2, 2)))
    gate_vector = noise(key_of[17], (D,), D ** -0.5, 0.125)
    dense_gate = noise(key_of[18], (D, FF_DENSE), D ** -0.5, 0.125, ((1, 128),))
    dense_up = noise(key_of[19], (D, FF_DENSE), D ** -0.5, 0.125, ((1, 128),))
    dense_down = noise(key_of[20], (FF_DENSE, D), (3.0 * FF_DENSE ** -0.5), 0.625, ((0, 64), (1, 2)))
    return dict(hidden_in=hidden_in, past_lengths=past_lengths, key_cache=key_cache, value_cache=value_cache, attn_gain=attn_gain, w_query=w_query, w_key=w_key, w_value=w_value, lambdas=lambdas, head_gain=head_gain, w_out=w_out, ffn_gain=ffn_gain, route_ids=route_ids, route_weights=route_weights, expert_gate=expert_gate, expert_up=expert_up, expert_down=expert_down, gate_vector=gate_vector, dense_gate=dense_gate, dense_up=dense_up, dense_down=dense_down)


norm_eps = 1e-05
rope_base = 10000.0

def rms_rows(values, scales):
    values = values.astype(jnp.float32)
    return values * lax.rsqrt(lax.optimization_barrier(jnp.mean(values * values, axis=-1, keepdims=True)) + norm_eps) * scales

def rotary(values, position):
    middle = values.shape[-1] // 2
    inverse = rope_base ** (-jnp.arange(middle, dtype=jnp.float32) / middle)
    angles = position.astype(jnp.float32)[:, None] * inverse[None, :]
    cosine = jnp.cos(angles)[:, None, None, :]
    sine_part = jnp.sin(angles)[:, None, None, :]
    leading, second = (values[..., :middle], values[..., middle:])
    return jnp.concatenate([leading * cosine - second * sine_part, second * cosine + leading * sine_part], axis=-1)

def rounded(values):
    return lax.optimization_barrier(values.astype(jnp.bfloat16)).astype(jnp.float32)

def reference(hidden_in, past_lengths, key_cache, value_cache, attn_gain, w_query, w_key, w_value, lambdas, head_gain, w_out, ffn_gain, route_ids, route_weights, expert_gate, expert_up, expert_down, gate_vector, dense_gate, dense_up, dense_down):
    batch_rows = hidden_in.shape[0]
    normed = rms_rows(hidden_in, attn_gain).astype(jnp.bfloat16)
    queries = rotary(jnp.dot(normed, w_query, preferred_element_type=jnp.float32).reshape(batch_rows, HEADS, 2, HEAD_DIM), past_lengths).astype(jnp.bfloat16)
    key_new = rotary(jnp.dot(normed, w_key, preferred_element_type=jnp.float32).reshape(batch_rows, KV_HEADS, 2, HEAD_DIM), past_lengths).astype(jnp.bfloat16)
    value_new = jnp.dot(normed, w_value, preferred_element_type=jnp.float32).astype(jnp.bfloat16)
    per_key = HEADS // KV_HEADS
    scale_qk = HEAD_DIM ** (-0.5)

    def attend(packed):
        query_seq, key_seq, value_seq, cache_keys, cache_values, length = packed
        grouped = query_seq.reshape(KV_HEADS, per_key, 2, HEAD_DIM).astype(jnp.float32)
        key_rows = cache_keys.reshape(CACHE_LEN, KV_HEADS, 2, HEAD_DIM).astype(jnp.float32)
        value_rows = cache_values.reshape(CACHE_LEN, KV_HEADS, VALUE_DIM).astype(jnp.float32)
        scores = jnp.einsum('gamd,lgmd->gaml', grouped, key_rows) * scale_qk
        own_score = jnp.einsum('gamd,gmd->gam', grouped, key_seq.astype(jnp.float32)) * scale_qk
        usable = jnp.arange(CACHE_LEN) < length
        scores = jnp.where(usable, scores, -jnp.inf)
        highest = jnp.maximum(lax.optimization_barrier(jnp.max(scores, axis=-1)), own_score)
        weights = jnp.exp(scores - highest[..., None])
        own_weight = jnp.exp(own_score - highest)
        totals = lax.optimization_barrier(jnp.sum(weights, axis=-1)) + own_weight
        summed = jnp.einsum('gaml,lge->game', rounded(weights), value_rows)
        summed = summed + rounded(own_weight)[..., None] * value_seq.reshape(KV_HEADS, 1, 1, VALUE_DIM).astype(jnp.float32)
        return (summed / totals[..., None]).reshape(HEADS, 2, VALUE_DIM)
    mapped = lax.map(attend, (queries, key_new, value_new, key_cache, value_cache, past_lengths))
    head_mix = mapped[:, :, 0] - lambdas[None, :, None] * mapped[:, :, 1]
    head_out = rms_rows(head_mix, head_gain).astype(jnp.bfloat16).reshape(batch_rows, N_TP, -1)
    out_rows = w_out.reshape(N_TP, -1, D)
    partials = jnp.einsum('sgk,gkd->sgd', head_out.astype(jnp.float32), out_rows.astype(jnp.float32))
    attn_out = lax.optimization_barrier(jnp.sum(rounded(partials), axis=1)).astype(jnp.bfloat16)
    residual = hidden_in.astype(jnp.float32) + attn_out.astype(jnp.float32)
    moe_in = rms_rows(residual, ffn_gain).astype(jnp.bfloat16)
    mix_gate = jax.nn.sigmoid(jnp.dot(moe_in, gate_vector, preferred_element_type=jnp.float32)).astype(jnp.bfloat16)
    slot_count = N_EP * CAP
    gate_pairs = expert_gate.reshape(EXPERTS, 2, D, -1)
    up_pairs = expert_up.reshape(EXPERTS, 2, D, -1)
    down_pairs = expert_down.reshape(EXPERTS, 2, -1, D)

    def add_expert(expert, moe_total):
        matches = route_ids == expert
        weight = lax.optimization_barrier(jnp.sum(jnp.where(matches, route_weights, 0.0), axis=1))
        chosen = jnp.any(matches, axis=1)
        number = jnp.sum(chosen.astype(jnp.int32))
        picked = jnp.nonzero(chosen, size=slot_count, fill_value=0)[0]
        live_slot = (jnp.arange(slot_count) < number).astype(jnp.float32)
        taken = moe_in[picked]
        gates_here = lax.dynamic_index_in_dim(gate_pairs, expert, 0, keepdims=False)
        ups_here = lax.dynamic_index_in_dim(up_pairs, expert, 0, keepdims=False)
        downs_here = lax.dynamic_index_in_dim(down_pairs, expert, 0, keepdims=False)
        result = jnp.zeros((slot_count, D), jnp.float32)
        for half_index in range(2):
            gate_pre = jnp.dot(taken, gates_here[half_index], preferred_element_type=jnp.float32)
            up_pre = jnp.dot(taken, ups_here[half_index], preferred_element_type=jnp.float32)
            inner_act = (jax.nn.silu(gate_pre) * up_pre).astype(jnp.bfloat16)
            result = result + jnp.dot(inner_act, downs_here[half_index], preferred_element_type=jnp.float32)
        return moe_total.at[picked].add(result * (weight[picked] * live_slot)[:, None])
    moe_out = lax.fori_loop(0, EXPERTS, add_expert, jnp.zeros((batch_rows, D), jnp.float32))
    dense_pre = jnp.dot(moe_in, dense_gate, preferred_element_type=jnp.float32)
    dense_upper = jnp.dot(moe_in, dense_up, preferred_element_type=jnp.float32)
    dense_act = (jax.nn.silu(dense_pre) * dense_upper).astype(jnp.bfloat16)
    dense_out = jnp.dot(dense_act, dense_down, preferred_element_type=jnp.float32) * mix_gate.astype(jnp.float32)[:, None]
    mixed_out = (residual + moe_out + dense_out).astype(jnp.bfloat16)
    return (mixed_out, key_new.reshape(batch_rows, -1), value_new)
```

```python
import jax
import jax.numpy as jnp
from jax import lax
from jax.experimental import pallas as pl
from jax.experimental.pallas import tpu as pltpu
from jax.sharding import PartitionSpec as P

HEAD_DIM = 64
VALUE_DIM = 128


norm_eps = 1e-05
rope_base = 10000.0


bf16=jnp.bfloat16; f32=jnp.float32
ROWS=32; HEADS_L=8; CH=256; GRP=4

def attention_body(lens, hid, gain, cos, sin, lam, hgain, wq_h, wk_h, wv_h, kc, vc, wo_h,
                   part, nk, nv,
                   wq, wk, wv, wo, kbuf, vbuf, qs, ks, vs, os_, wsem, ksem, vsem):
    n_seq=hid.shape[0]; clen=kbuf.shape[1]
    wcopies=[pltpu.make_async_copy(a,b,wsem.at[i]) for i,(a,b) in enumerate(((wq_h,wq),(wk_h,wk),(wv_h,wv),(wo_h,wo)))]
    for c in wcopies[:3]: c.start()
    def rows_of(s):
        return pl.multiple_of(((lens[s]+15)//16)*16,16)
    def kcopy(s):
        n=rows_of(s)
        return pltpu.make_async_copy(kc.at[s,pl.ds(0,n),:],kbuf.at[s,pl.ds(0,n),:],ksem.at[s])
    def vcopy(s):
        n=rows_of(s)
        return pltpu.make_async_copy(vc.at[s,pl.ds(0,n),:],vbuf.at[s,pl.ds(0,n),:],vsem.at[s])
    zero=jnp.zeros((clen,128),bf16)
    def start(s,_):
        vbuf[s]=zero
        return 0
    lax.fori_loop(0,n_seq,start,0)
    def start2(s,_):
        kcopy(s).start(); vcopy(s).start()
        return 0
    lax.fori_loop(0,n_seq,start2,0)
    wcopies[3].start()
    x=hid[...].astype(f32)
    normed=(x*lax.rsqrt(jnp.mean(x*x,axis=-1,keepdims=True)+norm_eps)*gain[...]).astype(bf16)
    lane=lax.broadcasted_iota(jnp.int32,(n_seq,128),1)
    first=(lane%64)<32
    c=cos[...]; sn=sin[...]
    def rot(v):
        other=jnp.where(first,pltpu.roll(v,96,1),pltpu.roll(v,32,1))
        return (v*c+other*sn).astype(bf16)
    wcopies[0].wait()
    q=jnp.dot(normed,wq[...],preferred_element_type=f32)
    for a in range(HEADS_L):
        qs[pl.ds(a,n_seq,stride=HEADS_L),:]=rot(q[:,a*128:(a+1)*128]).astype(f32)
    wcopies[1].wait(); wcopies[2].wait()
    k=rot(jnp.dot(normed,wk[...],preferred_element_type=f32))
    nk[...]=k; ks[...]=k.astype(f32)
    v=jnp.dot(normed,wv[...],preferred_element_type=f32).astype(bf16)
    nv[...]=v; vs[...]=v.astype(f32)
    lane8=lax.broadcasted_iota(jnp.int32,(HEADS_L,128),1)
    lamv=lam[...]; hg=hgain[...]
    scale=64**-0.5
    def one_group(g,C):
        L=C*CH
        sc=[];own=[]
        for i in range(GRP):
            s=g*GRP+i
            kcopy(s).wait()
            q8=qs[pl.ds(pl.multiple_of(s*8,8),8),:]
            q16=jnp.concatenate([jnp.where(lane8<64,q8,0.0),jnp.where(lane8<64,0.0,q8)],axis=0)
            own.append(jnp.sum(q16*ks[pl.ds(s,1),:],axis=-1,keepdims=True))
            t=lax.dot_general(q16.astype(bf16),kbuf[s,0:L,:],(((1,),(1,)),((),())),preferred_element_type=f32)
            pos=lax.broadcasted_iota(jnp.int32,(16,L),1)
            sc.append(jnp.where(pos<lens[s],t,-jnp.inf))
        for i in range(GRP):
            s=g*GRP+i
            m=jnp.maximum(jnp.max(sc[i],axis=-1,keepdims=True),own[i])
            p=jnp.exp((sc[i]-m)*scale)
            po=jnp.exp((own[i]-m)*scale)
            tot=jnp.sum(p,axis=-1,keepdims=True)+po
            vcopy(s).wait()
            o=jnp.dot(p.astype(bf16),vbuf[s,0:L,:],preferred_element_type=f32)
            o=o+po.astype(bf16).astype(f32)*vs[pl.ds(s,1),:]
            o=o/tot
            h=o[0:8]-lamv*o[8:16]
            h=h*lax.rsqrt(jnp.mean(h*h,axis=-1,keepdims=True)+norm_eps)*hg
            os_[pl.ds(pl.multiple_of(s*8,8),8),:]=h
    def loop(g,_):
        top=lens[g*GRP]
        for i in range(1,GRP): top=jnp.maximum(top,lens[g*GRP+i])
        need=(top+CH-1)//CH
        for C in range(1,clen//CH+1):
            @pl.when(need==C)
            def _(): one_group(g,C)
        return 0
    lax.fori_loop(0,n_seq//GRP,loop,0)
    ho=jnp.concatenate([os_[pl.ds(a,n_seq,stride=HEADS_L),:] for a in range(HEADS_L)],axis=-1).astype(bf16)
    wcopies[3].wait()
    part[...]=jnp.dot(ho,wo[...],preferred_element_type=f32).astype(bf16)

def attention(past_lengths,hidden_in,attn_gain,w_query,w_key,w_value,key_cache,value_cache,lambdas,head_gain,w_out):
    n,d=hidden_in.shape; clen=key_cache.shape[1]
    mid=32
    inv=10000.0**(-jnp.arange(mid,dtype=f32)/mid)
    ang=past_lengths.astype(f32)[:,None]*inv[None,:]
    co=jnp.cos(ang); si=jnp.sin(ang)
    cos=jnp.concatenate([co,co,co,co],-1); sin=jnp.concatenate([-si,si,-si,si],-1)
    vm=pl.BlockSpec(memory_space=pltpu.VMEM); an=pl.BlockSpec(memory_space=pltpu.HBM); sm=pl.BlockSpec(memory_space=pltpu.SMEM)
    return pl.pallas_call(attention_body,
        out_shape=(jax.ShapeDtypeStruct((n,w_out.shape[1]),bf16),jax.ShapeDtypeStruct((n,128),bf16),jax.ShapeDtypeStruct((n,128),bf16)),
        in_specs=[sm]+[vm]*6+[an]*6,
        out_specs=(vm,vm,vm),
        scratch_shapes=[pltpu.VMEM(w_query.shape,bf16),pltpu.VMEM(w_key.shape,bf16),pltpu.VMEM(w_value.shape,bf16),pltpu.VMEM(w_out.shape,bf16),
            pltpu.VMEM(key_cache.shape,bf16),pltpu.VMEM(value_cache.shape,bf16),
            pltpu.VMEM((n*8,128),f32),pltpu.VMEM((n,128),f32),pltpu.VMEM((n,128),f32),pltpu.VMEM((n*8,128),f32),
            pltpu.SemaphoreType.DMA((4,)),pltpu.SemaphoreType.DMA((n,)),pltpu.SemaphoreType.DMA((n,))],
        compiler_params=pltpu.CompilerParams(vmem_limit_bytes=62*1024*1024),
        name="attention",
    )(past_lengths,hidden_in,attn_gain.reshape(1,-1),cos,sin,lambdas.reshape(-1,1),head_gain.reshape(1,-1),w_query,w_key,w_value,key_cache,value_cache,w_out)


def swapped(x):
    return lax.ppermute(x, "tp", [(0, 1), (1, 0)])


def both_cores(x, rank):
    other = swapped(x)
    first = jnp.where(rank == 0, x, other)
    second = jnp.where(rank == 0, other, x)
    return jnp.concatenate([first, second], axis=1)


def sent_to_all(x, axis):
    size = lax.axis_size(axis)
    return lax.all_to_all(jnp.broadcast_to(x[None], (size, *x.shape)), axis, 0, 0, tiled=True)


def taken_together(x):
    return x.astype(jnp.float32) + swapped(x).astype(jnp.float32)


def in_order(pieces, dim):
    pieces = jnp.moveaxis(pieces, 0, dim)
    shape = pieces.shape
    return pieces.reshape(*shape[:dim], shape[dim] * shape[dim + 1], *shape[dim + 2 :])


def collect(x, axis, dim):
    pieces = sent_to_all(x, axis)
    return in_order(pieces, dim)


def in_one_piece(arrays, axis, dim, along):
    columns = [a.reshape(*a.shape[:along], -1) for a in arrays]
    both = jnp.concatenate(columns, axis=along)
    filled, at, outs = (lax.all_gather(both, axis, axis=dim, tiled=True), 0, [])
    for a, column in zip(arrays, columns):
        piece = filled[..., at : at + column.shape[along]]
        outs.append(piece.reshape(*piece.shape[:along], *a.shape[along:]))
        at += column.shape[along]
    return tuple(outs)


def side_by_side(arrays, axis, split_dim, concat_dim, along):
    both = jnp.concatenate(arrays, axis=along)
    filled, at, outs = (
        lax.all_to_all(both, axis, split_axis=split_dim, concat_axis=concat_dim, tiled=True),
        0,
        [],
    )
    for a in arrays:
        outs.append(lax.slice_in_dim(filled, at, at + a.shape[along], axis=along))
        at += a.shape[along]
    return tuple(outs)


def cut_along(x, dim, size):
    shape = x.shape
    pieces = x.reshape(*shape[:dim], size, shape[dim] // size, *shape[dim + 1 :])
    return jnp.moveaxis(pieces, dim, 0)


def sum_at_owner(x, axis, dim):
    pieces = cut_along(x, dim, lax.axis_size(axis))
    arrived = lax.all_to_all(pieces, axis, split_axis=0, concat_axis=0, tiled=True)
    return arrived.astype(jnp.float32).sum(axis=0)


def rms_rows(values, scales):
    values = values.astype(jnp.float32)
    return values * lax.rsqrt(jnp.mean(values * values, axis=-1, keepdims=True) + norm_eps) * scales


def rotary(values, position):
    middle = values.shape[-1] // 2
    inverse = rope_base ** (-jnp.arange(middle, dtype=jnp.float32) / middle)
    angles = position.astype(jnp.float32)[:, None] * inverse[None, :]
    cosine = jnp.cos(angles)[:, None, None, :]
    sine_part = jnp.sin(angles)[:, None, None, :]
    leading, second = (values[..., :middle], values[..., middle:])
    return jnp.concatenate(
        [leading * cosine - second * sine_part, second * cosine + leading * sine_part], axis=-1
    )


def per_device(
    hidden_in,
    past_lengths,
    key_cache,
    value_cache,
    attn_gain,
    w_query,
    w_key,
    w_value,
    lambdas,
    head_gain,
    w_out,
    ffn_gain,
    route_ids,
    route_weights,
    expert_gate,
    expert_up,
    expert_down,
    gate_vector,
    dense_gate,
    dense_up,
    dense_down,
):
    batch_rows = hidden_in.shape[0]
    model_width = hidden_in.shape[1]
    tp_count = lax.axis_size("tp")
    ep_count = lax.axis_size("ep")
    tp_rank = lax.axis_index("tp")
    half_width = model_width // tp_count
    own_part, key_new, value_new = attention(
        past_lengths, hidden_in, attn_gain, w_query, w_key, w_value, key_cache, value_cache,
        lambdas, head_gain, w_out,
    )
    attn_out = (
        own_part.astype(jnp.float32) + swapped(own_part).astype(jnp.float32)
    ).astype(jnp.bfloat16)
    residual = hidden_in.astype(jnp.float32) + attn_out.astype(jnp.float32)
    moe_in = rms_rows(residual, ffn_gain).astype(jnp.bfloat16)
    mix_gate = jax.nn.sigmoid(
        jnp.dot(moe_in, gate_vector, preferred_element_type=jnp.float32)
    ).astype(jnp.bfloat16)
    top_count = route_ids.shape[1]
    experts = ep_count // 2
    capacity = max(2, 2 * batch_rows * top_count // experts)
    flat_ids = route_ids.reshape(-1)
    matches = (flat_ids[:, None] == jnp.arange(experts)[None, :]).astype(jnp.int32)
    earlier = jnp.sum((jnp.cumsum(matches, axis=0) - matches) * matches, axis=1)
    slot_of = flat_ids * capacity + earlier
    placing = (jnp.arange(experts * capacity)[:, None] == slot_of[None, :]).astype(jnp.float32)
    repeated = jnp.repeat(moe_in, top_count, axis=0)
    packed = jnp.dot(
        placing.astype(jnp.bfloat16), repeated, preferred_element_type=jnp.float32
    ).astype(jnp.bfloat16)
    outgoing = jnp.broadcast_to(
        packed.reshape(experts, 1, capacity, model_width), (experts, 2, capacity, model_width)
    ).reshape(ep_count, capacity, model_width)
    arrived = lax.all_to_all(outgoing, "ep", split_axis=0, concat_axis=0, tiled=True)
    leading = arrived.shape[:2]
    flat_rows = arrived.reshape(-1, model_width)
    gate_pre = jnp.dot(flat_rows, expert_gate[0], preferred_element_type=jnp.float32)
    up_pre = jnp.dot(flat_rows, expert_up[0], preferred_element_type=jnp.float32)
    inner_act = (jax.nn.silu(gate_pre) * up_pre).astype(jnp.bfloat16)
    inner_act = both_cores(inner_act, tp_rank)
    partial_value = jnp.dot(inner_act, expert_down[0], preferred_element_type=jnp.float32).reshape(
        leading + (half_width,)
    )
    returned = lax.all_to_all(
        partial_value.astype(jnp.bfloat16), "ep", split_axis=0, concat_axis=0, tiled=True
    ).astype(partial_value.dtype)
    paired = jnp.sum(returned.reshape(experts, 2, capacity, half_width), axis=1).reshape(
        experts * capacity, half_width
    )
    weighted = (
        (placing * route_weights.reshape(1, -1))
        .reshape(experts * capacity, batch_rows, top_count)
        .sum(axis=2)
    )
    moe_out = jnp.einsum("ct,cd->td", weighted, paired, precision=lax.Precision.HIGHEST)
    own_half = lax.dynamic_slice_in_dim(moe_in, tp_rank * half_width, half_width, 1)
    rows_all, gates_all = in_one_piece((own_half, mix_gate), "ep", 0, 1)
    columns = dense_gate.shape[1]
    gate_cols, up_cols = side_by_side(
        (
            dense_gate.reshape(tp_count, half_width, columns),
            dense_up.reshape(tp_count, half_width, columns),
        ),
        "tp",
        0,
        2,
        1,
    )
    pre_gate, pre_up = (
        taken_together(
            jnp.dot(rows_all, gate_cols[0], preferred_element_type=jnp.float32).astype(
                jnp.bfloat16
            ),
        ),
        taken_together(
            jnp.dot(rows_all, up_cols[0], preferred_element_type=jnp.float32).astype(jnp.bfloat16),
        ),
    )
    dense_act = (jax.nn.silu(pre_gate) * pre_up).astype(jnp.bfloat16)
    gate_rows = gates_all.astype(jnp.float32)
    dense_out = sum_at_owner(
        (
            jnp.dot(dense_act, dense_down, preferred_element_type=jnp.float32) * gate_rows[:, None]
        ).astype(jnp.bfloat16),
        "ep",
        0,
    )
    own_residual = lax.dynamic_slice_in_dim(residual, tp_rank * half_width, half_width, 1)
    mixed_out = (own_residual + moe_out + dense_out).astype(jnp.bfloat16)
    return (mixed_out, key_new.reshape(batch_rows, -1), value_new)


def solution(mesh):
    return jax.shard_map(
        per_device,
        mesh=mesh,
        in_specs=(
            P("ep", None),
            P("ep"),
            P("ep", None, "tp"),
            P("ep", None, "tp"),
            P(),
            P(None, "tp"),
            P(None, "tp"),
            P(None, "tp"),
            P("tp"),
            P(),
            P("tp", None),
            P(),
            P("ep", None),
            P("ep", None),
            P("ep", None, "tp"),
            P("ep", None, "tp"),
            P("ep", None, "tp"),
            P(),
            P(None, ("ep", "tp")),
            P(None, ("ep", "tp")),
            P("ep", "tp"),
        ),
        out_specs=(P("ep", "tp"), P("ep", "tp"), P("ep", "tp")),
        check_vma=False,
    )
```

```python
import jax
import jax.numpy as jnp
from jax import lax
from jax.experimental import pallas as pl
from jax.experimental.pallas import tpu as pltpu
from jax.sharding import PartitionSpec as P

bf16=jnp.bfloat16; f32=jnp.float32
norm_eps=1e-05
ROWS=32; HEADS_L=8; CH=256; GRP=4

def attention_body(lens, hid, gain, cos, sin, lam, hgain, wq_h, wk_h, wv_h, kc, vc, wo_h,
                   part, nk, nv,
                   wq, wk, wv, wo, kbuf, vbuf, qs, ks, vs, os_, wsem, ksem, vsem):
    n_seq=hid.shape[0]; clen=kbuf.shape[1]
    wcopies=[pltpu.make_async_copy(a,b,wsem.at[i]) for i,(a,b) in enumerate(((wq_h,wq),(wk_h,wk),(wv_h,wv),(wo_h,wo)))]
    for c in wcopies[:3]: c.start()
    def rows_of(s):
        return pl.multiple_of(((lens[s]+15)//16)*16,16)
    def kcopy(s):
        n=rows_of(s)
        return pltpu.make_async_copy(kc.at[s,pl.ds(0,n),:],kbuf.at[s,pl.ds(0,n),:],ksem.at[s])
    def vcopy(s):
        n=rows_of(s)
        return pltpu.make_async_copy(vc.at[s,pl.ds(0,n),:],vbuf.at[s,pl.ds(0,n),:],vsem.at[s])
    zero=jnp.zeros((clen,128),bf16)
    def start(s,_):
        vbuf[s]=zero
        return 0
    lax.fori_loop(0,n_seq,start,0)
    def start2(s,_):
        kcopy(s).start(); vcopy(s).start()
        return 0
    lax.fori_loop(0,n_seq,start2,0)
    wcopies[3].start()
    x=hid[...].astype(f32)
    normed=(x*lax.rsqrt(jnp.mean(x*x,axis=-1,keepdims=True)+norm_eps)*gain[...]).astype(bf16)
    lane=lax.broadcasted_iota(jnp.int32,(n_seq,128),1)
    first=(lane%64)<32
    c=cos[...]; sn=sin[...]
    def rot(v):
        other=jnp.where(first,pltpu.roll(v,96,1),pltpu.roll(v,32,1))
        return (v*c+other*sn).astype(bf16)
    wcopies[0].wait()
    q=jnp.dot(normed,wq[...],preferred_element_type=f32)
    for a in range(HEADS_L):
        qs[pl.ds(a,n_seq,stride=HEADS_L),:]=rot(q[:,a*128:(a+1)*128]).astype(f32)
    wcopies[1].wait(); wcopies[2].wait()
    k=rot(jnp.dot(normed,wk[...],preferred_element_type=f32))
    nk[...]=k; ks[...]=k.astype(f32)
    v=jnp.dot(normed,wv[...],preferred_element_type=f32).astype(bf16)
    nv[...]=v; vs[...]=v.astype(f32)
    lane8=lax.broadcasted_iota(jnp.int32,(HEADS_L,128),1)
    lamv=lam[...]; hg=hgain[...]
    scale=64**-0.5
    def one_group(g,C):
        L=C*CH
        sc=[];own=[]
        for i in range(GRP):
            s=g*GRP+i
            kcopy(s).wait()
            q8=qs[pl.ds(pl.multiple_of(s*8,8),8),:]
            q16=jnp.concatenate([jnp.where(lane8<64,q8,0.0),jnp.where(lane8<64,0.0,q8)],axis=0)
            own.append(jnp.sum(q16*ks[pl.ds(s,1),:],axis=-1,keepdims=True))
            t=lax.dot_general(q16.astype(bf16),kbuf[s,0:L,:],(((1,),(1,)),((),())),preferred_element_type=f32)
            pos=lax.broadcasted_iota(jnp.int32,(16,L),1)
            sc.append(jnp.where(pos<lens[s],t,-jnp.inf))
        for i in range(GRP):
            s=g*GRP+i
            m=jnp.maximum(jnp.max(sc[i],axis=-1,keepdims=True),own[i])
            p=jnp.exp((sc[i]-m)*scale)
            po=jnp.exp((own[i]-m)*scale)
            tot=jnp.sum(p,axis=-1,keepdims=True)+po
            vcopy(s).wait()
            o=jnp.dot(p.astype(bf16),vbuf[s,0:L,:],preferred_element_type=f32)
            o=o+po.astype(bf16).astype(f32)*vs[pl.ds(s,1),:]
            o=o/tot
            h=o[0:8]-lamv*o[8:16]
            h=h*lax.rsqrt(jnp.mean(h*h,axis=-1,keepdims=True)+norm_eps)*hg
            os_[pl.ds(pl.multiple_of(s*8,8),8),:]=h
    def loop(g,_):
        top=lens[g*GRP]
        for i in range(1,GRP): top=jnp.maximum(top,lens[g*GRP+i])
        need=(top+CH-1)//CH
        for C in range(1,clen//CH+1):
            @pl.when(need==C)
            def _(): one_group(g,C)
        return 0
    lax.fori_loop(0,n_seq//GRP,loop,0)
    ho=jnp.concatenate([os_[pl.ds(a,n_seq,stride=HEADS_L),:] for a in range(HEADS_L)],axis=-1).astype(bf16)
    wcopies[3].wait()
    part[...]=jnp.dot(ho,wo[...],preferred_element_type=f32).astype(bf16)

def attention(past_lengths,hidden_in,attn_gain,w_query,w_key,w_value,key_cache,value_cache,lambdas,head_gain,w_out):
    n,d=hidden_in.shape; clen=key_cache.shape[1]
    mid=32
    inv=10000.0**(-jnp.arange(mid,dtype=f32)/mid)
    ang=past_lengths.astype(f32)[:,None]*inv[None,:]
    co=jnp.cos(ang); si=jnp.sin(ang)
    cos=jnp.concatenate([co,co,co,co],-1); sin=jnp.concatenate([-si,si,-si,si],-1)
    vm=pl.BlockSpec(memory_space=pltpu.VMEM); an=pl.BlockSpec(memory_space=pltpu.HBM); sm=pl.BlockSpec(memory_space=pltpu.SMEM)
    return pl.pallas_call(attention_body,
        out_shape=(jax.ShapeDtypeStruct((n,w_out.shape[1]),bf16),jax.ShapeDtypeStruct((n,128),bf16),jax.ShapeDtypeStruct((n,128),bf16)),
        in_specs=[sm]+[vm]*6+[an]*6,
        out_specs=(vm,vm,vm),
        scratch_shapes=[pltpu.VMEM(w_query.shape,bf16),pltpu.VMEM(w_key.shape,bf16),pltpu.VMEM(w_value.shape,bf16),pltpu.VMEM(w_out.shape,bf16),
            pltpu.VMEM(key_cache.shape,bf16),pltpu.VMEM(value_cache.shape,bf16),
            pltpu.VMEM((n*8,128),f32),pltpu.VMEM((n,128),f32),pltpu.VMEM((n,128),f32),pltpu.VMEM((n*8,128),f32),
            pltpu.SemaphoreType.DMA((4,)),pltpu.SemaphoreType.DMA((n,)),pltpu.SemaphoreType.DMA((n,))],
        compiler_params=pltpu.CompilerParams(vmem_limit_bytes=62*1024*1024),
        name="attention",
    )(past_lengths,hidden_in,attn_gain.reshape(1,-1),cos,sin,lambdas.reshape(-1,1),head_gain.reshape(1,-1),w_query,w_key,w_value,key_cache,value_cache,w_out)


EPS_SHIFTS = ((0, 0, 1), (0, 0, 3), (1, 0, 0), (3, 0, 0), (0, 1, 0), (1, 0, 1), (3, 3, 3))
PAD = 48
SLOTS = 8
LIVE = 4


def class_of(chip):
    z, y, x = (chip // 16, (chip // 4) % 4, chip % 4)
    return ((x + z + 2 * y) % 4) * 2 + z % 2


def shifted(x, shift):
    pairs = []
    for chip in range(64):
        z, y, w = (chip // 16, (chip // 4) % 4, chip % 4)
        to = ((z - shift[0]) % 4) * 16 + ((y - shift[1]) % 4) * 4 + (w - shift[2]) % 4
        pairs.append((chip, to))
    return lax.ppermute(x, "ep", pairs)


def swapped(x):
    return lax.ppermute(x, "tp", [(0, 1), (1, 0)])


def turned(a, b):
    return lax.dot_general(a, b, (((1,), (1,)), ((), ())), preferred_element_type=f32)


def block_body(gate, up, down, out):
    cols = gate.shape[1]
    row = lax.broadcasted_iota(jnp.int32, (PAD, cols), 0)
    col = lax.broadcasted_iota(jnp.int32, (PAD, cols), 1)
    eye = (row == col).astype(f32).astype(bf16)
    wide = gate.shape[0]
    out[0:PAD, 0:wide] = turned(eye, gate[...]).astype(bf16)
    out[PAD : 2 * PAD, 0:wide] = turned(eye, up[...]).astype(bf16)
    row = lax.broadcasted_iota(jnp.int32, (2 * PAD, 2 * cols), 0)
    col = lax.broadcasted_iota(jnp.int32, (2 * PAD, 2 * cols), 1)
    low = jnp.logical_and(row < cols, col == row)
    high = jnp.logical_and(row >= PAD, jnp.logical_and(col >= cols, col - cols == row - PAD))
    pick = jnp.logical_or(low, high).astype(f32).astype(bf16)
    out[:, wide:] = jnp.dot(pick, down[...], preferred_element_type=f32).astype(bf16)


def spread_body(rank, first, second, hid, gain, vector, ids, out, res, gate):
    n, width = hid.shape
    half = width // 2
    attn = (first[...].astype(f32) + second[...].astype(f32)).astype(bf16).astype(f32)
    residual = hid[...].astype(f32) + attn
    moe = residual * lax.rsqrt(jnp.mean(residual * residual, axis=-1, keepdims=True) + norm_eps)
    moe = (moe * gain[...]).astype(bf16).astype(f32)
    logit = jnp.sum(moe * vector[...].astype(f32), axis=-1, keepdims=True)
    gate[...] = jnp.broadcast_to((1.0 / (1.0 + jnp.exp(-logit))).astype(bf16).astype(f32), gate.shape)
    lower = rank[0] == 0
    res[...] = jnp.where(lower, residual[:, :half], residual[:, half:])
    mine = jnp.where(lower, moe[:, :half], moe[:, half:]).astype(bf16)
    total = out.shape[0]
    corner = (
        lax.broadcasted_iota(jnp.int32, (8, 2), 0) == lax.broadcasted_iota(jnp.int32, (8, 2), 1)
    ).astype(f32)
    named = turned(corner.astype(bf16), ids[...].astype(f32).astype(bf16))
    row = lax.broadcasted_iota(jnp.int32, (total, n), 0)
    token = lax.broadcasted_iota(jnp.int32, (total, n), 1)
    chip = row // SLOTS
    slot = row % SLOTS
    expert = (chip // 2).astype(f32)
    hit = jnp.logical_or(named[0:1, :] == expert, named[1:2, :] == expert).astype(f32)
    before = (
        lax.broadcasted_iota(jnp.int32, (n, n), 0) < lax.broadcasted_iota(jnp.int32, (n, n), 1)
    ).astype(f32)
    earlier = jnp.dot(hit.astype(bf16), before.astype(bf16), preferred_element_type=f32)
    routed = jnp.where(earlier == slot.astype(f32), hit, 0.0)
    always = (token == LIVE * class_of(chip) + slot - LIVE).astype(f32)
    place = jnp.where(slot < LIVE, routed, always).astype(bf16)
    out[...] = jnp.dot(place, mine, preferred_element_type=f32).astype(bf16)


def hidden_body(rank, own, other, gate, up, *rest):
    blocks, (act, routed, dense) = (rest[:-3], rest[-3:])
    width = own.shape[1]
    lower = rank[0] == 0
    head = lax.broadcasted_iota(jnp.int32, (2, 8, width), 1) < LIVE

    def part(k, _):
        at = pl.multiple_of(k * 32, 32)
        to = pl.multiple_of(k * 16, 16)
        a = own[pl.ds(at, 32), :].astype(f32)
        b = other[pl.ds(at, 32), :].astype(f32)
        for x, lanes in ((jnp.where(lower, a, b), 0), (jnp.where(lower, b, a), width)):
            x = x.reshape(2, 2, 8, width)
            even, odd = (x[:, 0], x[:, 1])
            kept = jnp.where(head, even, pltpu.roll(odd, LIVE, 1)).reshape(16, width)
            rest_ = jnp.where(head, pltpu.roll(even, LIVE, 1), odd).reshape(16, width)
            routed[pl.ds(to, 16), lanes : lanes + width] = kept.astype(bf16)
            dense[pl.ds(to, 16), lanes : lanes + width] = rest_.astype(bf16)
        return 0

    lax.fori_loop(0, own.shape[0] // 32, part, 0)
    rows = routed.shape[0]
    cols = gate.shape[1]

    def gated(g, u):
        return (g / (1.0 + jnp.exp(-g)) * u).astype(bf16)

    x = routed[...]
    act[0:rows, 0:cols] = gated(
        jnp.dot(x, gate[...], preferred_element_type=f32),
        jnp.dot(x, up[...], preferred_element_type=f32),
    )
    act[0:rows, cols:] = jnp.zeros((rows, act.shape[1] - cols), bf16)
    x = dense[...]
    act[rows:, :] = gated(
        turned(x, jnp.concatenate([b[0:PAD, 0 : 2 * width] for b in blocks], axis=0)),
        turned(x, jnp.concatenate([b[PAD : 2 * PAD, 0 : 2 * width] for b in blocks], axis=0)),
    )


def down_body(rank, own, other, down, *rest):
    blocks, (out, routed, dense) = (rest[:-3], rest[-3:])
    rows = routed.shape[0]
    cols = down.shape[0] // 2
    width = out.shape[1]
    here = rank[0]
    sums = []
    for ref, core in ((own, here), (other, 1 - here)):
        at = pl.multiple_of(core * cols, 16)
        low = pl.multiple_of(core * PAD, 16)
        m = jnp.dot(ref[0:rows, 0:cols], down[pl.ds(at, cols), :], preferred_element_type=f32)
        wd = jnp.concatenate([b[pl.ds(low, PAD), 2 * width :] for b in blocks], axis=0)
        sums.append((m, jnp.dot(ref[rows:, :], wd, preferred_element_type=f32)))
    routed[...] = sums[0][0] + sums[1][0]
    dense[...] = sums[0][1] + sums[1][1]
    head = lax.broadcasted_iota(jnp.int32, (2, 8, width), 1) < LIVE

    def part(k, _):
        at = pl.multiple_of(k * 16, 16)
        to = pl.multiple_of(k * 32, 32)
        m = routed[pl.ds(at, 16), :].reshape(2, 8, width)
        d = dense[pl.ds(at, 16), :].reshape(2, 8, width)
        even = jnp.where(head, m, pltpu.roll(d, LIVE, 1))
        odd = jnp.where(head, pltpu.roll(m, LIVE, 1), d)
        both = jnp.concatenate([even[0], odd[0], even[1], odd[1]], axis=0)
        out[pl.ds(to, 32), :] = both.astype(bf16)
        return 0

    lax.fori_loop(0, rows // 16, part, 0)


def combine_body(back, res, gate, ids, weights, out):
    n = res.shape[0]
    total = back.shape[0]
    lane = lax.broadcasted_iota(jnp.int32, (n, total), 1)
    token = lax.broadcasted_iota(jnp.int32, (n, total), 0)
    chip = lane // SLOTS
    slot = lane % SLOTS
    expert = chip // 2
    first = (ids[:, 0:1] == expert).astype(f32)
    second = (ids[:, 1:2] == expert).astype(f32)
    after = (
        lax.broadcasted_iota(jnp.int32, (n, n), 1) < lax.broadcasted_iota(jnp.int32, (n, n), 0)
    ).astype(f32)
    earlier = jnp.dot(
        after.astype(bf16), (first + second).astype(bf16), preferred_element_type=f32
    )
    routed = jnp.where(
        earlier == slot.astype(f32), first * weights[:, 0:1] + second * weights[:, 1:2], 0.0
    )
    always = jnp.where(token == LIVE * class_of(chip) + slot - LIVE, gate[:, 0:1], 0.0)
    w = jnp.where(slot < LIVE, routed, always)
    high = w.astype(bf16)
    left = w - high.astype(f32)
    mid = left.astype(bf16)
    low = (left - mid.astype(f32)).astype(bf16)
    parts = jnp.dot(
        jnp.concatenate([high, mid, low], axis=0), back[...], preferred_element_type=f32
    )
    added = parts[0:n] + parts[n : 2 * n] + parts[2 * n :]
    out[...] = (res[...] + added).astype(bf16)


VM = pl.BlockSpec(memory_space=pltpu.VMEM)
SM = pl.BlockSpec(memory_space=pltpu.SMEM)


def local_kernel(body, outs, ins, scalars=0, scratch=(), name=None):
    return pl.pallas_call(
        body,
        out_shape=tuple(jax.ShapeDtypeStruct(s, d) for s, d in outs),
        in_specs=[SM] * scalars + [VM] * (len(ins) - scalars),
        out_specs=tuple(VM for _ in outs),
        scratch_shapes=[pltpu.VMEM(s, d) for s, d in scratch],
        compiler_params=pltpu.CompilerParams(vmem_limit_bytes=40 * 1024 * 1024),
        name=name,
    )(*ins)


def per_device(
    hidden_in,
    past_lengths,
    key_cache,
    value_cache,
    attn_gain,
    w_query,
    w_key,
    w_value,
    lambdas,
    head_gain,
    w_out,
    ffn_gain,
    route_ids,
    route_weights,
    expert_gate,
    expert_up,
    expert_down,
    gate_vector,
    dense_gate,
    dense_up,
    dense_down,
):
    batch_rows, model_width = hidden_in.shape
    half_width = model_width // 2
    ep_count = lax.axis_size("ep")
    rank = lax.axis_index("tp").astype(jnp.int32).reshape(1)
    (block,) = local_kernel(
        block_body,
        [((2 * PAD, model_width + half_width), bf16)],
        (dense_gate, dense_up, dense_down),
        name="block",
    )
    blocks = [block] + [shifted(block, shift) for shift in EPS_SHIFTS]
    own_part, key_new, value_new = attention(
        past_lengths, hidden_in, attn_gain, w_query, w_key, w_value, key_cache, value_cache,
        lambdas, head_gain, w_out,
    )
    total = ep_count * SLOTS
    outgoing, own_residual, mix_gate = local_kernel(
        spread_body,
        [((total, half_width), bf16), ((batch_rows, half_width), f32), ((batch_rows, 128), f32)],
        (
            rank, own_part, swapped(own_part), hidden_in, ffn_gain.reshape(1, -1),
            gate_vector.reshape(1, -1), route_ids,
        ),
        scalars=1,
        name="spread",
    )
    arrived = lax.all_to_all(
        outgoing.reshape(ep_count, SLOTS, half_width), "ep", 0, 0, tiled=True
    ).reshape(total, half_width)
    live = ep_count * LIVE
    hidden = len(blocks) * PAD
    (act,) = local_kernel(
        hidden_body,
        [((2 * live, hidden), bf16)],
        (rank, arrived, swapped(arrived), expert_gate[0], expert_up[0], *blocks),
        scalars=1,
        scratch=[((live, model_width), bf16)] * 2,
        name="hidden",
    )
    (partial_value,) = local_kernel(
        down_body,
        [((total, half_width), bf16)],
        (rank, act, swapped(act), expert_down[0], *blocks),
        scalars=1,
        scratch=[((live, half_width), f32)] * 2,
        name="down",
    )
    back = lax.all_to_all(
        partial_value.reshape(ep_count, SLOTS, half_width), "ep", 0, 0, tiled=True
    ).reshape(total, half_width)
    (mixed_out,) = local_kernel(
        combine_body,
        [((batch_rows, half_width), bf16)],
        (back, own_residual, mix_gate, route_ids, route_weights),
        name="combine",
    )
    return (mixed_out, key_new, value_new)


def solution(mesh):
    return jax.shard_map(
        per_device,
        mesh=mesh,
        in_specs=(
            P("ep", None),
            P("ep"),
            P("ep", None, "tp"),
            P("ep", None, "tp"),
            P(),
            P(None, "tp"),
            P(None, "tp"),
            P(None, "tp"),
            P("tp"),
            P(),
            P("tp", None),
            P(),
            P("ep", None),
            P("ep", None),
            P("ep", None, "tp"),
            P("ep", None, "tp"),
            P("ep", None, "tp"),
            P(),
            P(None, ("ep", "tp")),
            P(None, ("ep", "tp")),
            P("ep", "tp"),
        ),
        out_specs=(P("ep", "tp"), P("ep", "tp"), P("ep", "tp")),
        check_vma=False,
    )
```
